32 devices in a mesh: sp: 8 (over z, y), tp: 4 (over x, core).
Axes of the slice: x: 2, y: 2, z: 4, core: 2. Of those that a mesh axis runs over, the one named last changes fastest.
Arguments:
- hidden: bfloat16 [6144, 2048], P(('sp', 'tp')), may hold values from -24 to 24
- w_query: bfloat16 [2048, 1536], P(None, 'tp'), may hold values from -0.125 to 0.125
- w_latent: bfloat16 [2048, 512], replicated, may hold values from -0.125 to 0.125
- w_rotary: bfloat16 [2048, 32], replicated, may hold values from -0.125 to 0.125
- latent_gain: float32 [512], replicated, may hold values from 0.1 to 1.9
- w_expand: bfloat16 [512, 2048], P(None, 'tp'), may hold values from -0.25 to 0.25
- w_rquery: bfloat16 [2048, 1024], P(None, 'tp'), may hold values from -0.125 to 0.125
- w_rkey: bfloat16 [2048, 1024], P(None, 'tp'), may hold values from -0.125 to 0.125
- w_rvalue: bfloat16 [2048, 1024], P(None, 'tp'), may hold values from -0.125 to 0.125
- w_rgate: bfloat16 [2048, 1024], P(None, 'tp'), may hold values from -0.125 to 0.125
- retention_gain: float32 [1024], P('tp'), may hold values from 0.1 to 1.9
- log_decay: float32 [2, 8, 6144], P(None, 'tp', 'sp'), may hold values from -0.6 to 0
- w_out: bfloat16 [2048, 2048], replicated, may hold values from -0.125 to 0.125
Outputs:
- mixed: bfloat16 [6144, 2048], P(('sp', 'tp'))
- log_total: float32 [16, 6144], P('tp', 'sp')
The draws below stay inside these ranges and needn't reach their ends.
All inputs are finite; a program needn't handle non-finite values.
Results may differ from the reference program's by a relative error of at most 0.015.
Values may be sent and summed in bfloat16 or wider, within the bound.
No kernel may reach another device: no remote copies, remote signals or barrier semaphores. Data moves between devices by JAX's collectives and lax.ppermute only.
A program may use at most 192 MiB of HBM per device.

```python
import math
from functools import partial
import jax
import jax.numpy as jnp
from jax import lax

D = 2048
HM = 16
KVR = 512
NOPE = 64
ROPE = 32
VH = 64
HR = 8
DK = 128
DV = 128
RBLK = 128
TOK_DEV = 768
SEQUENCE_LENGTH = 6144
MIXW = 2048


def draw_hidden(key, part):
    base_key = jax.random.fold_in(jax.random.fold_in(key, 11), 0)
    entries = jnp.clip(jax.random.normal(base_key, (SEQUENCE_LENGTH, D), jnp.float32), -6.0, 6.0)
    return entries.astype(jnp.bfloat16)


def draw_log_decay(key, part):
    initial_seed, latter_seed, quick_seed, gradual_seed, segment_seed, compartment_seed, surge_seed, tertiary_seed, objective_seed = jax.random.split(jax.random.fold_in(key, 23), 9)
    ranking = jnp.stack([jax.random.permutation(initial_seed, HR), jax.random.permutation(latter_seed, HR)])
    fast_count = HR // 2
    quick_markers = (ranking < fast_count)[:, :, None]
    fast_speed = jax.random.uniform(quick_seed, (2, HR, 1), jnp.float32, 1.0 / 100.0, 1.0 / 30.0)
    slow_speed = jax.random.uniform(gradual_seed, (2, HR, 1), jnp.float32, 0.05, 0.25) * math.log(10.0) / SEQUENCE_LENGTH
    block_factor = jnp.exp(jax.random.uniform(segment_seed, (2, HR, SEQUENCE_LENGTH // TOK_DEV), jnp.float32, math.log(0.5), math.log(2.0)))
    block_factor = jnp.repeat(block_factor, TOK_DEV, axis=2)
    cell_factor = jax.random.uniform(compartment_seed, (2, HR, SEQUENCE_LENGTH), jnp.float32, 0.5, 1.5)
    velocity_amounts = jnp.where(quick_markers, fast_speed, slow_speed) * block_factor * cell_factor
    surge_locations = jnp.stack([jax.random.permutation(surge_seed, SEQUENCE_LENGTH)[:2], jax.random.permutation(tertiary_seed, SEQUENCE_LENGTH)[:2]])
    objective_amounts = jax.random.uniform(objective_seed, (2, 2, 1), jnp.float32, 0.2, 0.35)
    surge_matches = jnp.arange(SEQUENCE_LENGTH)[None, None, :] == surge_locations[:, :, None]
    surge_occurrences = jnp.sum(jnp.where(surge_matches, jnp.log(1.0 - objective_amounts), 0.0), axis=1)
    return -velocity_amounts + jnp.where(quick_markers, 0.0, surge_occurrences[:, None, :])


def shard_levels(key, dims, cuts, least, largest):
    level, own = 1.0, jax.random.fold_in(key, 6)
    for dim, shards_of in cuts:
        steps = jnp.exp(jax.random.uniform(jax.random.fold_in(own, dim), (shards_of,), jnp.float32, least / len(cuts), largest / len(cuts)))
        level = level * jnp.repeat(steps, dims[dim] // shards_of).reshape([-1 if axis == dim else 1 for axis in range(len(dims))])
    return level


def bell_draw(rng, extent, width, limit, cuts=(), held_as=jnp.bfloat16):
    array = width * jax.random.normal(rng, extent, jnp.float32)
    if cuts:
        array = array * shard_levels(rng, extent, cuts, -0.22, 0.18)
    return jnp.clip(array, -limit, limit).astype(held_as)


def setup_inputs(seed: int = 0) -> dict:
    keys = jax.random.split(jax.random.key(seed), 14)
    hidden = draw_hidden(jax.random.fold_in(keys[13], 71), 0)
    w_query = bell_draw(keys[1], (D, HM * (NOPE + ROPE)), D ** -0.5, 0.125, ((1, 4),))
    w_latent = bell_draw(keys[2], (D, KVR), D ** -0.5, 0.125)
    w_rotary = bell_draw(keys[3], (D, ROPE), D ** -0.5, 0.125)
    latent_gain = jnp.clip(1.0 + 0.18 * jax.random.normal(keys[4], (KVR,), jnp.float32), 0.1, 1.9)
    w_expand = bell_draw(keys[5], (KVR, HM * (NOPE + VH)), KVR ** -0.5, 0.25, ((1, 4),))
    w_rquery = bell_draw(keys[6], (D, HR * DK), D ** -0.5, 0.125, ((1, 4),))
    w_rkey = bell_draw(keys[7], (D, HR * DK), D ** -0.5, 0.125, ((1, 4),))
    w_rvalue = bell_draw(keys[8], (D, HR * DV), D ** -0.5, 0.125, ((1, 4),))
    w_rgate = bell_draw(keys[9], (D, HR * DV), D ** -0.5, 0.125, ((1, 4),))
    retention_gain = jnp.clip(1.0 + 0.18 * jax.random.normal(keys[10], (HR * DV,), jnp.float32), 0.1, 1.9)
    log_decay = draw_log_decay(jax.random.fold_in(keys[13], 71), 0)
    w_out = bell_draw(keys[12], (MIXW, D), MIXW ** -0.5, 0.125)
    return dict(hidden=hidden, w_query=w_query, w_latent=w_latent, w_rotary=w_rotary, latent_gain=latent_gain, w_expand=w_expand, w_rquery=w_rquery, w_rkey=w_rkey, w_rvalue=w_rvalue, w_rgate=w_rgate, retention_gain=retention_gain, log_decay=log_decay, w_out=w_out)


eps = 1e-06
rope_base = 10000.0
highest = lax.Precision.HIGHEST

def rotate(values, places):
    turn_width = values.shape[-1]
    inverse = rope_base ** (-jnp.arange(0, turn_width, 2, dtype=jnp.float32) / turn_width)
    angles = places[:, None] * inverse[None, :]
    cosine = jnp.cos(angles)[:, None, :]
    sine_part = jnp.sin(angles)[:, None, :]
    leading, trailing = jnp.split(values, 2, axis=-1)
    return jnp.concatenate([leading * cosine - trailing * sine_part, leading * sine_part + trailing * cosine], axis=-1)

def retain(queries, key_rows, values, log_rate, strict):
    length = queries.shape[0]
    blocks = length // RBLK
    offsets = jnp.arange(RBLK)
    if strict:
        allowed = offsets[:, None] > offsets[None, :]
    else:
        allowed = offsets[:, None] >= offsets[None, :]

    def advance(carried_state, inputs):
        block_query, segment_seed, block_value, block_rate = inputs
        running = jnp.cumsum(block_rate)
        spread = jnp.where(allowed, running[:, None] - running[None, :], 0.0)
        damping = jnp.where(allowed, jnp.exp(spread), 0.0)
        scores = jnp.dot(block_query, segment_seed.T, precision=highest) * damping
        within = jnp.dot(scores, block_value, precision=highest)
        carried = jnp.exp(running)[:, None] * jnp.dot(block_query, carried_state, precision=highest)
        fading = jnp.exp(running[-1] - running)[:, None]
        next_state = jnp.exp(running[-1]) * carried_state + jnp.dot((segment_seed * fading).T, block_value, precision=highest)
        return (next_state, within + carried)
    initial = jnp.zeros((queries.shape[1], values.shape[1]), jnp.float32)
    last_state, outputs = lax.scan(advance, initial, (queries.reshape(blocks, RBLK, -1), key_rows.reshape(blocks, RBLK, -1), values.reshape(blocks, RBLK, -1), log_rate.reshape(blocks, RBLK)))
    return (last_state, outputs.reshape(length, -1))

def attend_head(inputs):
    head_query, head_key, head_value = inputs
    tokens = head_query.shape[0]
    key_full = head_key.astype(jnp.float32)
    value_full = head_value.astype(jnp.float32)
    score_scale = (NOPE + ROPE) ** (-0.5)

    def one_block(block_query):
        scores = jnp.dot(block_query.astype(jnp.float32), key_full.T, precision=highest) * score_scale
        row_peak = lax.optimization_barrier(jnp.max(scores, axis=1, keepdims=True))
        weights = jnp.exp(scores - row_peak)
        weight_sum = lax.optimization_barrier(jnp.sum(weights, axis=1, keepdims=True))
        rounded = lax.optimization_barrier(weights.astype(jnp.bfloat16))
        mixed_rows = jnp.dot(rounded.astype(jnp.float32), value_full, precision=highest) / weight_sum
        return (mixed_rows.astype(jnp.bfloat16), (row_peak + jnp.log(weight_sum))[:, 0])
    mixed_rows, logsum = lax.map(one_block, head_query.reshape(tokens // TOK_DEV, TOK_DEV, -1))
    return (mixed_rows.reshape(tokens, -1), logsum.reshape(tokens))

def reference(hidden, w_query, w_latent, w_rotary, latent_gain, w_expand, w_rquery, w_rkey, w_rvalue, w_rgate, retention_gain, log_decay, w_out):
    tokens = hidden.shape[0]
    places = jnp.arange(tokens, dtype=jnp.float32)

    def project(weight):
        return jnp.dot(hidden, weight, preferred_element_type=jnp.float32)
    query_raw = project(w_query).reshape(tokens, HM, NOPE + ROPE)
    queries = jnp.concatenate([query_raw[..., :NOPE], rotate(query_raw[..., NOPE:], places)], axis=-1).astype(jnp.bfloat16)
    latent_raw = project(w_latent)
    latent = (latent_raw * lax.rsqrt(lax.optimization_barrier(jnp.mean(latent_raw * latent_raw, axis=1, keepdims=True)) + eps) * latent_gain).astype(jnp.bfloat16)
    key_turned = rotate(project(w_rotary)[:, None, :], places)[:, 0, :].astype(jnp.bfloat16)
    expanded = jnp.dot(latent, w_expand, preferred_element_type=jnp.float32).astype(jnp.bfloat16).reshape(tokens, HM, NOPE + VH)
    keys_all = jnp.concatenate([expanded[..., :NOPE], jnp.broadcast_to(key_turned[:, None, :], (tokens, HM, ROPE))], axis=-1)
    head_rows, log_total = lax.map(attend_head, (queries.transpose(1, 0, 2), keys_all.transpose(1, 0, 2), expanded[..., NOPE:].transpose(1, 0, 2)))
    attention_out = head_rows.transpose(1, 0, 2).reshape(tokens, HM * VH)
    ret_query = rotate(project(w_rquery).reshape(tokens, HR, DK), places).astype(jnp.bfloat16)
    ret_key = (rotate(project(w_rkey).reshape(tokens, HR, DK), places) * DK ** (-0.5)).astype(jnp.bfloat16)
    ret_value = project(w_rvalue).astype(jnp.bfloat16).reshape(tokens, HR, DV)
    gate_raw = project(w_rgate).astype(jnp.bfloat16)
    head_query = ret_query.astype(jnp.float32).transpose(1, 0, 2)
    head_key = ret_key.astype(jnp.float32).transpose(1, 0, 2)
    head_value = ret_value.astype(jnp.float32).transpose(1, 0, 2)
    forward = jax.vmap(partial(retain, strict=False))(head_query, head_key, head_value, log_decay[0])[1]
    backward = jax.vmap(partial(retain, strict=True))(jnp.flip(head_query, 1), jnp.flip(head_key, 1), jnp.flip(head_value, 1), jnp.flip(log_decay[1], 1))[1]
    combined = forward + jnp.flip(backward, 1)
    centre = lax.optimization_barrier(jnp.mean(combined, axis=2, keepdims=True))
    variance = lax.optimization_barrier(jnp.mean(jnp.square(combined - centre), axis=2, keepdims=True))
    normed = ((combined - centre) * lax.rsqrt(variance + eps)).transpose(1, 0, 2).reshape(tokens, HR * DV)
    retention_out = (normed * retention_gain * jax.nn.silu(gate_raw.astype(jnp.float32))).astype(jnp.bfloat16)
    joined = jnp.concatenate([attention_out, retention_out], axis=1)
    mixed = jnp.dot(joined, w_out, preferred_element_type=jnp.float32).astype(jnp.bfloat16)
    return (mixed, log_total)
```

```python
import math

import jax
import jax.numpy as jnp
from jax import lax
from jax.experimental import pallas as pl
from jax.experimental.pallas import tpu as pltpu
from jax.sharding import PartitionSpec as P

NOPE = 64
ROPE = 32
VH = 64
DK = 128
DV = 128
LANES = 128

eps = 1e-06
rope_base = 10000.0


def turn_tables(width, places):
    inverse = rope_base ** (-jnp.arange(0, width, 2, dtype=jnp.float32) / width)
    angles = places[:, None] * inverse[None, :]
    return jnp.cos(angles), jnp.sin(angles)


def rotate(values, cosine, sine):
    leading, trailing = jnp.split(values, 2, axis=-1)
    return jnp.concatenate(
        [leading * cosine - trailing * sine, leading * sine + trailing * cosine], axis=-1
    )


def attention_kernel(heads, chunks, block, *refs):
    q_ref, wk_ref, wv_ref = refs[:3]
    chunk_refs = refs[3 : 3 + chunks]
    o_ref, kt_ref, v_ref = refs[3 + chunks :]
    head = pl.program_id(0)
    rows = chunk_refs[0].shape[0]
    width = NOPE + ROPE

    @pl.when((head == 0) & (pl.program_id(1) == 0))
    def _():
        for number, ref in enumerate(chunk_refs):
            at = slice(number * rows, (number + 1) * rows)
            message = ref[...]
            keys = lax.dot_general(
                wk_ref[...], message, (((1,), (1,)), ((), ())), preferred_element_type=jnp.float32
            ).astype(jnp.bfloat16)
            values = jnp.dot(
                message, wv_ref[...], preferred_element_type=jnp.float32
            ).astype(jnp.bfloat16)
            for h in range(heads):
                kt_ref[h, :, at] = keys[h * width : (h + 1) * width]
                v_ref[h, at, :] = values[:, h * LANES : (h + 1) * LANES]

    query = q_ref[0]
    total = kt_ref.shape[2]

    def scores_of(number):
        return jnp.dot(
            query,
            kt_ref[head, :, number * block : (number + 1) * block],
            preferred_element_type=jnp.float32,
        )

    steps = total // block
    scores = scores_of(0)
    peak = accumulated = None
    for number in range(steps):
        following = scores_of(number + 1) if number + 1 < steps else None
        block_peak = jnp.max(scores, axis=1, keepdims=True)
        new_peak = block_peak if peak is None else jnp.maximum(peak, block_peak)
        weights = jnp.exp2(scores - new_peak).astype(jnp.bfloat16)
        added = jnp.dot(
            weights,
            v_ref[head, number * block : (number + 1) * block, :],
            preferred_element_type=jnp.float32,
        )
        if peak is None:
            accumulated = added
        else:
            accumulated = accumulated * jnp.exp2(peak - new_peak) + added
        peak = new_peak
        scores = following
    weight_sum = accumulated[:, VH : VH + 1]
    log_total = peak * math.log(2.0) + jnp.log(weight_sum)
    lane = lax.broadcasted_iota(jnp.int32, accumulated.shape, 1)
    o_ref[0] = jnp.where(lane < VH, accumulated / weight_sum, log_total)


def attend(query, key_weight, value_weight, messages):
    heads, rows, width = query.shape
    total = sum(message.shape[0] for message in messages)
    tile = math.gcd(rows, 256)
    block = math.gcd(total, 1024)

    def whole(array):
        return pl.BlockSpec(array.shape, lambda h, i: (0, 0))

    return pl.pallas_call(
        lambda *refs: attention_kernel(heads, len(messages), block, *refs),
        grid=(heads, rows // tile),
        in_specs=[
            pl.BlockSpec((1, tile, width), lambda h, i: (h, i, 0)),
            whole(key_weight),
            whole(value_weight),
        ]
        + [whole(message) for message in messages],
        out_specs=pl.BlockSpec((1, tile, LANES), lambda h, i: (h, i, 0)),
        out_shape=jax.ShapeDtypeStruct((heads, rows, LANES), jnp.float32),
        scratch_shapes=[
            pltpu.VMEM((heads, width, total), jnp.bfloat16),
            pltpu.VMEM((heads, total, LANES), jnp.bfloat16),
        ],
        compiler_params=pltpu.CompilerParams(
            dimension_semantics=("arbitrary", "arbitrary"), vmem_limit_bytes=56 * 1024 * 1024
        ),
        name="attend",
    )(query, key_weight, value_weight, *messages)


def split_three(values):
    high = lax.reduce_precision(values, 8, 7)
    middle = lax.reduce_precision(values - high, 8, 7)
    low = values - high - middle
    return jnp.stack([high, middle, low]).astype(jnp.bfloat16)


def local(
    hidden,
    w_query,
    w_latent,
    w_rotary,
    latent_gain,
    w_expand,
    w_rquery,
    w_rkey,
    w_rvalue,
    w_rgate,
    retention_gain,
    log_decay,
    w_out,
):
    sp, tp = lax.axis_size("sp"), lax.axis_size("tp")
    sp_mine, tp_mine = lax.axis_index("sp"), lax.axis_index("tp")
    own_rows, model = hidden.shape
    rows = own_rows * tp
    heads = w_query.shape[1] // (NOPE + ROPE)
    ret_heads = w_rquery.shape[1] // DK
    latent_width = w_latent.shape[1]

    def from_peer(x, k):
        return lax.ppermute(x, "tp", [(t, t ^ k) for t in range(tp)])

    peer = tp_mine ^ jnp.arange(tp)
    spots = (peer[:, None] * own_rows + jnp.arange(own_rows)[None, :]).reshape(rows)
    places = (sp_mine * rows + spots).astype(jnp.float32)

    own_latent = jnp.dot(hidden, w_latent, preferred_element_type=jnp.float32)
    own_latent = (
        own_latent
        * lax.rsqrt(jnp.mean(own_latent * own_latent, axis=1, keepdims=True) + eps)
        * latent_gain
    ).astype(jnp.bfloat16)
    own_turned = rotate(
        jnp.dot(hidden, w_rotary, preferred_element_type=jnp.float32),
        *turn_tables(ROPE, places[:own_rows]),
    ).astype(jnp.bfloat16)
    message_width = -(-(latent_width + ROPE + 1) // LANES) * LANES
    own_message = jnp.concatenate(
        [
            own_latent,
            own_turned,
            jnp.ones((own_rows, 1), jnp.bfloat16),
            jnp.zeros((own_rows, message_width - latent_width - ROPE - 1), jnp.bfloat16),
        ],
        axis=1,
    )
    lane_message = jnp.concatenate(
        [own_message] + [from_peer(own_message, k) for k in range(2, tp, 2)], axis=0
    )
    pieces = [hidden] + [None] * (tp - 1)
    for k in range(2, tp, 2):
        pieces[k] = from_peer(hidden, k)
    for k in range(1, tp, 2):
        pieces[k] = from_peer(pieces[k - 1], 1)
    messages = [lane_message] + [
        lax.ppermute(lane_message, "sp", [(s, (s + shift) % sp) for s in range(sp)])
        for shift in range(1, sp)
    ]
    messages = messages + [from_peer(message, 1) for message in messages]

    expand = w_expand.reshape(latent_width, heads, NOPE + VH)
    eye = jnp.broadcast_to(jnp.eye(ROPE, dtype=jnp.bfloat16)[:, None, :], (ROPE, heads, ROPE))
    key_weight = jnp.concatenate(
        [
            jnp.pad(expand[..., :NOPE], ((0, 0), (0, 0), (0, ROPE))),
            jnp.pad(eye, ((0, 0), (0, 0), (NOPE, 0))),
            jnp.zeros((message_width - latent_width - ROPE, heads, NOPE + ROPE), jnp.bfloat16),
        ],
        axis=0,
    )
    key_weight = key_weight.reshape(message_width, heads * (NOPE + ROPE)).T
    one_row = jnp.broadcast_to(
        (jnp.arange(LANES) == VH).astype(jnp.bfloat16)[None, None], (1, heads, LANES)
    )
    value_weight = jnp.concatenate(
        [
            jnp.pad(expand[..., NOPE:], ((0, 0), (0, 0), (0, LANES - VH))),
            jnp.zeros((ROPE, heads, LANES), jnp.bfloat16),
            one_row,
            jnp.zeros((message_width - latent_width - ROPE - 1, heads, LANES), jnp.bfloat16),
        ],
        axis=0,
    ).reshape(message_width, heads * LANES)

    weights = jnp.concatenate([w_rquery, w_rkey, w_rvalue, w_rgate, w_query], axis=1)
    borders = [0]
    for weight in (w_rquery, w_rkey, w_rvalue, w_rgate, w_query):
        borders.append(borders[-1] + weight.shape[1])
    projected = jnp.concatenate(
        [jnp.dot(piece, weights, preferred_element_type=jnp.float32) for piece in pieces], axis=0
    )
    rquery_raw, rkey_raw, rvalue_raw, rgate_raw, query_raw = [
        projected[:, borders[n] : borders[n + 1]] for n in range(5)
    ]

    cosine, sine = turn_tables(DK, places)

    def turned_heads(raw, factor):
        return [
            (rotate(raw[:, h * DK : (h + 1) * DK], cosine, sine) * factor).astype(jnp.bfloat16)
            for h in range(ret_heads)
        ]

    ret_query = jnp.stack(turned_heads(rquery_raw, 1.0))
    ret_key = jnp.stack(turned_heads(rkey_raw, DK ** (-0.5)))
    ret_value = jnp.stack(
        [rvalue_raw[:, h * DV : (h + 1) * DV].astype(jnp.bfloat16) for h in range(ret_heads)]
    )
    running = jnp.cumsum(log_decay, axis=2)
    totals = running[:, :, -1]
    exclusive = running - log_decay

    def by_peer(values):
        return values.reshape(ret_heads, tp, own_rows)[:, peer].reshape(ret_heads, rows)

    ahead = by_peer(running[0])
    behind = by_peer(exclusive[1])
    ahead_key = jnp.exp(totals[0][:, None] - ahead)
    behind_key = jnp.exp(behind)
    key_full = ret_key.astype(jnp.float32)
    faded = jnp.concatenate(
        [key_full * ahead_key[..., None], key_full * behind_key[..., None]], axis=2
    ).astype(jnp.bfloat16)
    states = jnp.einsum(
        "hmd,hme->hde", faded, ret_value, preferred_element_type=jnp.float32
    ).astype(jnp.bfloat16)
    total_rows = jnp.pad(
        split_three(totals.reshape(-1)), ((0, 13), (0, LANES - 2 * ret_heads))
    )
    sent = jnp.concatenate([states.reshape(ret_heads * 2 * DK, DV), total_rows], axis=0)
    gathered = lax.all_to_all(
        jnp.broadcast_to(sent[None], (sp,) + sent.shape), "sp", split_axis=0, concat_axis=0
    )
    everywhere = (
        gathered[:, -16:-13, : 2 * ret_heads].astype(jnp.float32).sum(axis=1)
    ).reshape(sp, 2, ret_heads)
    number = jnp.arange(sp)
    between_ahead = (number[None, :] > number[:, None]) & (number[None, :] < sp_mine)
    between_behind = (number[None, :] < number[:, None]) & (number[None, :] > sp_mine)
    gain_ahead = jnp.where(
        (number < sp_mine)[:, None],
        jnp.exp(jnp.sum(jnp.where(between_ahead[..., None], everywhere[None, :, 0], 0.0), axis=1)),
        0.0,
    )
    gain_behind = jnp.where(
        (number > sp_mine)[:, None],
        jnp.exp(jnp.sum(jnp.where(between_behind[..., None], everywhere[None, :, 1], 0.0), axis=1)),
        0.0,
    )
    gains = jnp.stack([gain_ahead, gain_behind], axis=2)
    entering = jnp.sum(
        gathered[:, :-16].astype(jnp.float32).reshape(sp, ret_heads, 2, DK, DV)
        * gains[..., None, None],
        axis=0,
    ).astype(jnp.bfloat16)

    spread = jnp.where(
        spots[:, None] >= spots[None, :],
        ahead[:, :, None] - ahead[:, None, :],
        behind[:, None, :] - behind[:, :, None],
    )
    near = jnp.einsum("hnd,hmd->hnm", ret_query, ret_key, preferred_element_type=jnp.float32)
    near = (near * jnp.exp(spread)).astype(jnp.bfloat16)
    combined = jnp.einsum("hnm,hme->hne", near, ret_value, preferred_element_type=jnp.float32)
    ahead_query = jnp.exp(ahead)
    behind_query = jnp.exp(totals[1][:, None] - behind)
    combined = (
        combined
        + ahead_query[..., None]
        * jnp.einsum(
            "hnd,hde->hne", ret_query, entering[:, 0], preferred_element_type=jnp.float32
        )
        + behind_query[..., None]
        * jnp.einsum(
            "hnd,hde->hne", ret_query, entering[:, 1], preferred_element_type=jnp.float32
        )
    )
    centre = jnp.mean(combined, axis=2, keepdims=True)
    variance = jnp.mean(jnp.square(combined - centre), axis=2, keepdims=True)
    normed = (combined - centre) * lax.rsqrt(variance + eps)
    normed = jnp.concatenate([normed[h] for h in range(ret_heads)], axis=1)
    gate = rgate_raw.astype(jnp.bfloat16).astype(jnp.float32)
    retention_out = (normed * retention_gain * jax.nn.silu(gate)).astype(jnp.bfloat16)

    def to_owners(mixer):
        blocks = mixer.reshape(tp, own_rows, mixer.shape[1])
        return [blocks[0]] + [from_peer(blocks[k], k) for k in range(1, tp)]

    retention_all = to_owners(retention_out)

    scale = (NOPE + ROPE) ** (-0.5) * math.log2(math.e)
    shaped = query_raw.reshape(rows, heads, NOPE + ROPE).transpose(1, 0, 2) * scale
    query = jnp.concatenate(
        [shaped[..., :NOPE], rotate(shaped[..., NOPE:], *turn_tables(ROPE, places))], axis=2
    ).astype(jnp.bfloat16)
    attended = attend(query, key_weight, value_weight, messages)
    attention_out = jnp.concatenate(
        [attended[h, :, :VH].astype(jnp.bfloat16) for h in range(heads)], axis=1
    )
    log_total = attended[:, :, VH].reshape(heads, tp, own_rows)[:, peer].reshape(heads, rows)
    attention_all = to_owners(attention_out)

    split = attention_out.shape[1] * tp
    out_attention = w_out[:split].reshape(tp, -1, model)[peer].reshape(split, model)
    out_retention = w_out[split:].reshape(tp, -1, model)[peer].reshape(-1, model)
    mixed = jnp.dot(
        jnp.concatenate(retention_all, axis=1), out_retention, preferred_element_type=jnp.float32
    ) + jnp.dot(
        jnp.concatenate(attention_all, axis=1), out_attention, preferred_element_type=jnp.float32
    )
    return (mixed.astype(jnp.bfloat16), log_total)


def solution(mesh):
    return jax.shard_map(
        local,
        mesh=mesh,
        in_specs=(
            P(("sp", "tp"), None),
            P(None, "tp"),
            P(),
            P(),
            P(),
            P(None, "tp"),
            P(None, "tp"),
            P(None, "tp"),
            P(None, "tp"),
            P(None, "tp"),
            P("tp"),
            P(None, "tp", "sp"),
            P(),
        ),
        out_specs=(P(("sp", "tp"), None), P("tp", "sp")),
        check_vma=False,
    )
```

```python
import math

import jax
import jax.numpy as jnp
from jax import lax
from jax.experimental import pallas as pl
from jax.experimental.pallas import tpu as pltpu
from jax.sharding import PartitionSpec as P

NOPE = 64
ROPE = 32
VH = 64
DK = 128
DV = 128
LANES = 128

eps = 1e-06
rope_base = 10000.0


def turn_tables(width, places):
    inverse = rope_base ** (-jnp.arange(0, width, 2, dtype=jnp.float32) / width)
    angles = places[:, None] * inverse[None, :]
    return jnp.cos(angles), jnp.sin(angles)


def rotate(values, cosine, sine):
    leading, trailing = jnp.split(values, 2, axis=-1)
    return jnp.concatenate(
        [leading * cosine - trailing * sine, leading * sine + trailing * cosine], axis=-1
    )


def attention_kernel(heads, chunks, block, *refs):
    q_ref, wt_ref, w_ref = refs[:3]
    chunk_refs = refs[3 : 3 + chunks]
    o_ref, kt_ref, v_ref = refs[3 + chunks :]
    head = pl.program_id(0)
    rows = chunk_refs[0].shape[0]
    latent_width = w_ref.shape[0]

    @pl.when((head == 0) & (pl.program_id(1) == 0))
    def _():
        lane = lax.broadcasted_iota(jnp.int32, (rows, heads * LANES), 1)
        first = jnp.where(lane % LANES == 0, 1.0, 0.0)
        spot = (ROPE, chunk_refs[0].shape[1] - latent_width)
        pick = jnp.where(
            lax.broadcasted_iota(jnp.int32, spot, 0) == lax.broadcasted_iota(jnp.int32, spot, 1),
            1.0,
            0.0,
        ).astype(jnp.bfloat16)
        for number, ref in enumerate(chunk_refs):
            at = slice(number * rows, (number + 1) * rows)
            latent = ref[:, :latent_width]
            keys = lax.dot_general(
                wt_ref[...], latent, (((1,), (1,)), ((), ())), preferred_element_type=jnp.float32
            ).astype(jnp.bfloat16)
            turned = lax.dot_general(
                pick, ref[:, latent_width:], (((1,), (1,)), ((), ())),
                preferred_element_type=jnp.float32,
            ).astype(jnp.bfloat16)
            values = jnp.where(
                lane % LANES < NOPE,
                first,
                jnp.dot(latent, w_ref[...], preferred_element_type=jnp.float32),
            ).astype(jnp.bfloat16)
            for h in range(heads):
                kt_ref[h, :NOPE, at] = keys[h * LANES : h * LANES + NOPE]
                kt_ref[h, NOPE:, at] = turned
                v_ref[h, at, :] = values[:, h * LANES : (h + 1) * LANES]

    query = q_ref[0]
    total = kt_ref.shape[2]

    def scores_of(number):
        return jnp.dot(
            query,
            kt_ref[head, :, number * block : (number + 1) * block],
            preferred_element_type=jnp.float32,
        )

    steps = total // block
    scores = scores_of(0)
    peak = accumulated = None
    for number in range(steps):
        following = scores_of(number + 1) if number + 1 < steps else None
        block_peak = jnp.max(scores, axis=1, keepdims=True)
        new_peak = block_peak if peak is None else jnp.maximum(peak, block_peak)
        weights = jnp.exp2(scores - new_peak).astype(jnp.bfloat16)
        added = jnp.dot(
            weights,
            v_ref[head, number * block : (number + 1) * block, :],
            preferred_element_type=jnp.float32,
        )
        if peak is None:
            accumulated = added
        else:
            accumulated = accumulated * jnp.exp2(peak - new_peak) + added
        peak = new_peak
        scores = following
    weight_sum = accumulated[:, :1]
    log_total = peak * math.log(2.0) + jnp.log(weight_sum)
    lane = lax.broadcasted_iota(jnp.int32, accumulated.shape, 1)
    o_ref[0] = jnp.where(lane >= NOPE, accumulated / weight_sum, log_total)


def attend(query, expand_turned, expand, messages):
    heads, rows, width = query.shape
    total = sum(message.shape[0] for message in messages)
    tile = math.gcd(rows, 256)
    block = math.gcd(total, 1024)

    def whole(array):
        return pl.BlockSpec(array.shape, lambda h, i: (0, 0))

    return pl.pallas_call(
        lambda *refs: attention_kernel(heads, len(messages), block, *refs),
        grid=(heads, rows // tile),
        in_specs=[
            pl.BlockSpec((1, tile, width), lambda h, i: (h, i, 0)),
            whole(expand_turned),
            whole(expand),
        ]
        + [whole(message) for message in messages],
        out_specs=pl.BlockSpec((1, tile, LANES), lambda h, i: (h, i, 0)),
        out_shape=jax.ShapeDtypeStruct((heads, rows, LANES), jnp.float32),
        scratch_shapes=[
            pltpu.VMEM((heads, width, total), jnp.bfloat16),
            pltpu.VMEM((heads, total, LANES), jnp.bfloat16),
        ],
        compiler_params=pltpu.CompilerParams(
            dimension_semantics=("arbitrary", "arbitrary"), vmem_limit_bytes=56 * 1024 * 1024
        ),
        name="attend",
    )(query, expand_turned, expand, *messages)


def split_three(values):
    high = lax.reduce_precision(values, 8, 7)
    middle = lax.reduce_precision(values - high, 8, 7)
    low = values - high - middle
    return jnp.stack([high, middle, low]).astype(jnp.bfloat16)


def local(
    hidden,
    w_query,
    w_latent,
    w_rotary,
    latent_gain,
    w_expand,
    w_rquery,
    w_rkey,
    w_rvalue,
    w_rgate,
    retention_gain,
    log_decay,
    w_out,
):
    sp, tp = lax.axis_size("sp"), lax.axis_size("tp")
    sp_mine, tp_mine = lax.axis_index("sp"), lax.axis_index("tp")
    own_rows, model = hidden.shape
    rows = own_rows * tp
    heads = w_query.shape[1] // (NOPE + ROPE)
    ret_heads = w_rquery.shape[1] // DK
    latent_width = w_latent.shape[1]

    def from_peer(x, k):
        return lax.ppermute(x, "tp", [(t, t ^ k) for t in range(tp)])

    peer = tp_mine ^ jnp.arange(tp)
    spots = (peer[:, None] * own_rows + jnp.arange(own_rows)[None, :]).reshape(rows)
    places = (sp_mine * rows + spots).astype(jnp.float32)

    own_latent = jnp.dot(hidden, w_latent, preferred_element_type=jnp.float32)
    own_latent = (
        own_latent
        * lax.rsqrt(jnp.mean(own_latent * own_latent, axis=1, keepdims=True) + eps)
        * latent_gain
    ).astype(jnp.bfloat16)
    own_turned = rotate(
        jnp.dot(hidden, w_rotary, preferred_element_type=jnp.float32),
        *turn_tables(ROPE, places[:own_rows]),
    ).astype(jnp.bfloat16)
    message_width = latent_width + LANES
    own_message = jnp.concatenate(
        [
            own_latent,
            own_turned,
            jnp.zeros((own_rows, LANES - ROPE), jnp.bfloat16),
        ],
        axis=1,
    )
    lane_message = jnp.concatenate(
        [own_message] + [from_peer(own_message, k) for k in range(2, tp, 2)], axis=0
    )
    lane_message, w_out, w_expand = lax.optimization_barrier((lane_message, w_out, w_expand))
    pieces = [hidden] + [None] * (tp - 1)
    for k in range(2, tp, 2):
        pieces[k] = from_peer(hidden, k)
    for k in range(1, tp, 2):
        pieces[k] = from_peer(pieces[k - 1], 1)
    messages = [lane_message] + [
        lax.ppermute(lane_message, "sp", [(s, (s + shift) % sp) for s in range(sp)])
        for shift in range(1, sp)
    ]

    expand_turned = w_expand.T

    weights = jnp.concatenate([w_rquery, w_rkey, w_rvalue, w_rgate, w_query], axis=1)
    borders = [0]
    for weight in (w_rquery, w_rkey, w_rvalue, w_rgate, w_query):
        borders.append(borders[-1] + weight.shape[1])
    block = w_out.shape[0] // (2 * tp)
    out_weight = jnp.concatenate(
        [
            lax.dynamic_slice_in_dim(w_out, (mixer * tp + (tp_mine ^ k)) * block, block, 0)
            for mixer in range(2)
            for k in range(tp)
        ],
        axis=0,
    )
    pieces[tp - 1], out_weight, expand_turned = lax.optimization_barrier(
        (pieces[tp - 1], out_weight, expand_turned)
    )
    projected = jnp.concatenate(
        [jnp.dot(piece, weights, preferred_element_type=jnp.float32) for piece in pieces], axis=0
    )
    rquery_raw, rkey_raw, rvalue_raw, rgate_raw, query_raw = [
        projected[:, borders[n] : borders[n + 1]] for n in range(5)
    ]

    cosine, sine = turn_tables(DK, places)

    def turned_heads(raw, factor):
        return [
            (rotate(raw[:, h * DK : (h + 1) * DK], cosine, sine) * factor).astype(jnp.bfloat16)
            for h in range(ret_heads)
        ]

    ret_query = jnp.stack(turned_heads(rquery_raw, 1.0))
    ret_key = jnp.stack(turned_heads(rkey_raw, DK ** (-0.5)))
    ret_value = jnp.stack(
        [rvalue_raw[:, h * DV : (h + 1) * DV].astype(jnp.bfloat16) for h in range(ret_heads)]
    )
    running = jnp.cumsum(log_decay, axis=2)
    totals = running[:, :, -1]
    exclusive = running - log_decay

    def by_peer(values):
        return values.reshape(ret_heads, tp, own_rows)[:, peer].reshape(ret_heads, rows)

    ahead = by_peer(running[0])
    behind = by_peer(exclusive[1])
    ahead_key = jnp.exp(totals[0][:, None] - ahead)
    behind_key = jnp.exp(behind)
    key_full = ret_key.astype(jnp.float32)
    faded = jnp.concatenate(
        [key_full * ahead_key[..., None], key_full * behind_key[..., None]], axis=2
    ).astype(jnp.bfloat16)
    states = jnp.einsum(
        "hmd,hme->hde", faded, ret_value, preferred_element_type=jnp.float32
    ).astype(jnp.bfloat16)
    total_rows = jnp.pad(
        split_three(totals.reshape(-1)), ((0, 13), (0, LANES - 2 * ret_heads))
    )
    sent = jnp.concatenate([states.reshape(ret_heads * 2 * DK, DV), total_rows], axis=0)
    *messages, sent = lax.optimization_barrier((*messages, sent))
    messages = messages + [from_peer(message, 1) for message in messages]
    gathered = lax.all_to_all(
        jnp.broadcast_to(sent[None], (sp,) + sent.shape), "sp", split_axis=0, concat_axis=0
    )
    everywhere = (
        gathered[:, -16:-13, : 2 * ret_heads].astype(jnp.float32).sum(axis=1)
    ).reshape(sp, 2, ret_heads)
    number = jnp.arange(sp)
    between_ahead = (number[None, :] > number[:, None]) & (number[None, :] < sp_mine)
    between_behind = (number[None, :] < number[:, None]) & (number[None, :] > sp_mine)
    gain_ahead = jnp.where(
        (number < sp_mine)[:, None],
        jnp.exp(jnp.sum(jnp.where(between_ahead[..., None], everywhere[None, :, 0], 0.0), axis=1)),
        0.0,
    )
    gain_behind = jnp.where(
        (number > sp_mine)[:, None],
        jnp.exp(jnp.sum(jnp.where(between_behind[..., None], everywhere[None, :, 1], 0.0), axis=1)),
        0.0,
    )
    gains = jnp.stack([gain_ahead, gain_behind], axis=2)
    entering = jnp.sum(
        gathered[:, :-16].astype(jnp.float32).reshape(sp, ret_heads, 2, DK, DV)
        * gains[..., None, None],
        axis=0,
    ).astype(jnp.bfloat16)

    spread = jnp.where(
        spots[:, None] >= spots[None, :],
        ahead[:, :, None] - ahead[:, None, :],
        behind[:, None, :] - behind[:, :, None],
    )
    near = jnp.einsum("hnd,hmd->hnm", ret_query, ret_key, preferred_element_type=jnp.float32)
    near = (near * jnp.exp(spread)).astype(jnp.bfloat16)
    combined = jnp.einsum("hnm,hme->hne", near, ret_value, preferred_element_type=jnp.float32)
    ahead_query = jnp.exp(ahead)
    behind_query = jnp.exp(totals[1][:, None] - behind)
    combined = (
        combined
        + ahead_query[..., None]
        * jnp.einsum(
            "hnd,hde->hne", ret_query, entering[:, 0], preferred_element_type=jnp.float32
        )
        + behind_query[..., None]
        * jnp.einsum(
            "hnd,hde->hne", ret_query, entering[:, 1], preferred_element_type=jnp.float32
        )
    )
    centre = jnp.mean(combined, axis=2, keepdims=True)
    variance = jnp.mean(jnp.square(combined - centre), axis=2, keepdims=True)
    normed = (combined - centre) * lax.rsqrt(variance + eps)
    normed = jnp.concatenate([normed[h] for h in range(ret_heads)], axis=1)
    gate = rgate_raw.astype(jnp.bfloat16).astype(jnp.float32)
    retention_out = (normed * retention_gain * jax.nn.silu(gate)).astype(jnp.bfloat16)

    def to_owners(mixer):
        blocks = mixer.reshape(tp, own_rows, mixer.shape[1])
        return [blocks[0]] + [from_peer(blocks[k], k) for k in range(1, tp)]

    scale = (NOPE + ROPE) ** (-0.5) * math.log2(math.e)
    shaped = query_raw.reshape(rows, heads, NOPE + ROPE).transpose(1, 0, 2) * scale
    query = jnp.concatenate(
        [shaped[..., :NOPE], rotate(shaped[..., NOPE:], *turn_tables(ROPE, places))], axis=2
    ).astype(jnp.bfloat16)
    query, retention_out = lax.optimization_barrier((query, retention_out))
    retention_all = to_owners(retention_out)
    attended = attend(query, expand_turned, w_expand, messages)
    attention_out = jnp.concatenate(
        [attended[h, :, NOPE:].astype(jnp.bfloat16) for h in range(heads)], axis=1
    )
    log_total = attended[:, :, 0].reshape(heads, tp, own_rows)[:, peer].reshape(heads, rows)
    attention_all = to_owners(attention_out)

    split = attention_out.shape[1] * tp
    mixed = jnp.dot(
        jnp.concatenate(retention_all, axis=1),
        out_weight[split:],
        preferred_element_type=jnp.float32,
    ) + jnp.dot(
        jnp.concatenate(attention_all, axis=1),
        out_weight[:split],
        preferred_element_type=jnp.float32,
    )
    return (mixed.astype(jnp.bfloat16), log_total)


def solution(mesh):
    return jax.shard_map(
        local,
        mesh=mesh,
        in_specs=(
            P(("sp", "tp"), None),
            P(None, "tp"),
            P(),
            P(),
            P(),
            P(None, "tp"),
            P(None, "tp"),
            P(None, "tp"),
            P(None, "tp"),
            P(None, "tp"),
            P("tp"),
            P(None, "tp", "sp"),
            P(),
        ),
        out_specs=(P(("sp", "tp"), None), P("tp", "sp")),
        check_vma=False,
    )
```
